32 devices in a mesh: ra: 8 (over z, y), cb: 4 (over x, core).
Axes of the slice: x: 2, y: 2, z: 4, core: 2. Of those that a mesh axis runs over, the one named last changes fastest.
Arguments:
- tokens: bfloat16 [512, 4096], P(None, 'ra'), may hold values from -4 to 4, as said below
- pre_gain_first: float32 [4096], P('ra'), may hold values from 0.1 to 1.9
- gate_first: bfloat16 [4096, 11264], P('ra', 'cb'), may hold values from -0.125 to 0.125
- up_first: bfloat16 [4096, 11264], P('ra', 'cb'), may hold values from -0.125 to 0.125
- down_first: bfloat16 [11264, 4096], P('cb', 'ra'), may hold values from -0.078125 to 0.078125
- post_gain_first: float32 [4096], P('ra'), may hold values from 0.1 to 1.9
- pre_gain_second: float32 [4096], P('ra'), may hold values from 0.1 to 1.9
- gate_second: bfloat16 [4096, 11264], P('ra', 'cb'), may hold values from -0.125 to 0.125
- up_second: bfloat16 [4096, 11264], P('ra', 'cb'), may hold values from -0.125 to 0.125
- down_second: bfloat16 [11264, 4096], P('cb', 'ra'), may hold values from -0.078125 to 0.078125
- post_gain_second: float32 [4096], P('ra'), may hold values from 0.1 to 1.9
Outputs:
- mixed: bfloat16 [512, 4096], P(None, 'ra')
The draws below stay inside these ranges and needn't reach their ends.
Inputs may be any that keep to these rules, and one draw needn't show every extreme that they name: `tokens`: each block of 128 consecutive channels has its own scale, and rows have their own scales.
All inputs are finite; a program needn't handle non-finite values.
Results may differ from the reference program's by a relative error of at most 0.0071.
Values may be sent and summed in bfloat16 or wider, within the bound.
A program may use at most 64 MiB of HBM per device.

```python
import jax
import jax.numpy as jnp
from jax import lax

D = 4096
FF = 11264
TOKENS = 512


def draw_tokens(key, part):
    base_key = jax.random.fold_in(key, 11)
    key_noise, key_block, key_row, key_common = jax.random.split(base_key, 4)
    noise = jax.random.normal(key_noise, (TOKENS, D), jnp.float32)
    block_scale = jnp.exp(jax.random.uniform(key_block, (32,), jnp.float32, jnp.log(0.15), jnp.log(0.6)))
    column_scale = jnp.repeat(block_scale, D // 32)
    row_scale = jax.random.uniform(key_row, (TOKENS, 1), jnp.float32, 0.7, 1.4)
    values = noise * column_scale[None, :] * row_scale
    return jnp.clip(values, -4.0, 4.0).astype(jnp.bfloat16)


def spiked(drawn, key, source, target, parts, factor):
    owner, partner = [(jnp.arange(drawn.shape[dim]) // (drawn.shape[dim] // parts)).reshape([-1 if axis == dim else 1 for axis in range(drawn.ndim)]) for dim in (source, target)]
    chosen = jax.random.permutation(key, parts)[partner]
    strong = (owner == chosen) | (owner == (partner + parts // 2) % parts)
    return jnp.where(strong, factor * drawn, drawn)


def level_of(own_key, shape, cuts, low, top_value):
    factor_of = 1.0
    for position, blocks in cuts:
        heights = jax.random.uniform(jax.random.fold_in(jax.random.fold_in(own_key, 6), position), (blocks,), jnp.float32, low / len(cuts), top_value / len(cuts))
        factor_of = factor_of * jnp.repeat(jnp.exp(heights), shape[position] // blocks).reshape((-1,) + (1,) * (len(shape) - 1 - position))
    return factor_of


def gaussian_with(key, dims, spread, bound, cuts, heavy, kind=jnp.bfloat16):
    result = spread * jax.random.normal(key, dims, jnp.float32)
    if cuts:
        result = result * level_of(key, dims, cuts, -0.22, 0.18)
    return jnp.clip(spiked(result, jax.random.fold_in(key, 3), *heavy), -bound, bound).astype(kind)


def setup_inputs(seed: int = 0) -> dict:
    arg_keys = jax.random.split(jax.random.key(seed), 12)
    tokens = draw_tokens(jax.random.fold_in(arg_keys[11], 71), 0)
    pre_gain_first = jnp.clip(1.0 + 0.18 * jax.random.normal(arg_keys[1], (D,), jnp.float32), 0.1, 1.9)
    gate_first = gaussian_with(arg_keys[2], (D, FF), D ** -0.5, 0.125, ((0, 8), (1, 4)), (0, 1, 8, 2.0))
    up_first = gaussian_with(arg_keys[3], (D, FF), D ** -0.5, 0.125, ((0, 8), (1, 4)), (0, 1, 8, 2.0))
    down_first = gaussian_with(arg_keys[4], (FF, D), FF ** -0.5, 0.078125, ((0, 4), (1, 8)), (0, 1, 8, 2.0))
    post_gain_first = jnp.clip(1.0 + 0.18 * jax.random.normal(arg_keys[5], (D,), jnp.float32), 0.1, 1.9)
    pre_gain_second = jnp.clip(1.0 + 0.18 * jax.random.normal(arg_keys[6], (D,), jnp.float32), 0.1, 1.9)
    gate_second = gaussian_with(arg_keys[7], (D, FF), D ** -0.5, 0.125, ((0, 8), (1, 4)), (0, 1, 8, 2.0))
    up_second = gaussian_with(arg_keys[8], (D, FF), D ** -0.5, 0.125, ((0, 8), (1, 4)), (0, 1, 8, 2.0))
    down_second = gaussian_with(arg_keys[9], (FF, D), FF ** -0.5, 0.078125, ((0, 4), (1, 8)), (0, 1, 8, 2.0))
    post_gain_second = jnp.clip(1.0 + 0.18 * jax.random.normal(arg_keys[10], (D,), jnp.float32), 0.1, 1.9)
    return dict(tokens=tokens, pre_gain_first=pre_gain_first, gate_first=gate_first, up_first=up_first, down_first=down_first, post_gain_first=post_gain_first, pre_gain_second=pre_gain_second, gate_second=gate_second, up_second=up_second, down_second=down_second, post_gain_second=post_gain_second)


EPS = 1e-06

def row_scale(values):
    return lax.rsqrt(lax.optimization_barrier(jnp.mean(values * values, axis=-1, keepdims=True)) + EPS)

def half_step(resid, pre_gain, gate_weight, up_weight, down_weight, post_gain):
    normed = (resid * row_scale(resid) * pre_gain).astype(jnp.bfloat16)
    gate_value = jnp.dot(normed, gate_weight, preferred_element_type=jnp.float32)
    up_value = jnp.dot(normed, up_weight, preferred_element_type=jnp.float32)
    hidden = (jax.nn.silu(gate_value) * up_value).astype(jnp.bfloat16)
    branch = jnp.dot(hidden, down_weight, preferred_element_type=jnp.float32)
    return resid + 0.5 * branch * row_scale(branch) * post_gain

def reference(tokens, pre_gain_first, gate_first, up_first, down_first, post_gain_first, pre_gain_second, gate_second, up_second, down_second, post_gain_second):
    resid = tokens.astype(jnp.float32)
    middle = half_step(resid, pre_gain_first, gate_first, up_first, down_first, post_gain_first)
    final = half_step(middle, pre_gain_second, gate_second, up_second, down_second, post_gain_second)
    return final.astype(jnp.bfloat16)
```

```python
import functools

import jax
import jax.numpy as jnp
from jax import lax
from jax.experimental import pallas as pl
from jax.experimental.pallas import tpu as pltpu
from jax.sharding import PartitionSpec as P

EPS = 1e-06
MESH = pl.DeviceIdType.MESH
F32 = jnp.float32
BF16 = jnp.bfloat16
LY, LZ = 3, 3
POST = (2, 3, 2, 3)


def log2(n):
    return n.bit_length() - 1


def spread(col):
    return jnp.broadcast_to(col, (col.shape[0], 128)).T[0:8]


def column(row):
    return jnp.broadcast_to(row[0:1], (128, row.shape[1])).T


class Plan:
    def __init__(self, n, nc, tokens, depth, hidden):
        self.n, self.nc, self.tokens, self.depth = n, nc, tokens, depth
        self.ny = 1 << (log2(n) // 2)
        self.nz = n // self.ny
        self.kx = log2(nc) - 1
        self.tb = 64 * self.ny
        self.half, self.g = self.tb // 2, 16
        self.cw = 256 if hidden % 256 == 0 else 128
        self.chunks, self.blocks = hidden // self.cw, tokens // self.tb
        self.items = self.chunks * self.blocks
        self.act = (self.nz - 1) * LZ + LY
        self.down = self.act + LY + (self.nz - 1) * LZ
        steps = [0, POST[0]] + [POST[1]] * self.kx + [POST[2], POST[3]]
        self.post = [self.down + sum(steps[: i + 1]) for i in range(len(steps))]
        self.gap = max(0, self.chunks + self.post[-1] - self.items)
        self.ticks = 2 * self.items + self.gap + self.post[-1]


def kernel(p, width, *refs):
    (tok, pre1, post1, pre2, post2, gate1, up1, down1, gate2, up2, down2, y_out), refs = refs[:12], refs[12:]
    (both_v, down_v, h_v, mid, acc, branch, scale, hid), refs = refs[:8], refs[8:]
    (y1_snd, y1_rcv, ca_snd, ca_rcv, cb_snd, cb_rcv, y2_snd, y2_rcv), refs = refs[:8], refs[8:]
    (d_rcv, x_snd, x_rcv, tot, br_snd, br_rcv, ms_snd, ms_rcv), refs = refs[:8], refs[8:]
    (w_sem, y1_s, y1_r, ca_s, ca_r, cb_s, cb_r, y2_s, y2_r, h2_s, h2_r, ga_s, ga_r, gb_s, gb_r, h1_s, h1_r), refs = (
        refs[:17], refs[17:],
    )
    d_s, d_r, x_s, x_r, t_s, t_r, br_s, br_r, ms_s, ms_r = refs

    n, nc, ny, nz, tb, half, g, cw = p.n, p.nc, p.ny, p.nz, p.tb, p.half, p.g, p.cw
    chunks, blocks, items = p.chunks, p.blocks, p.items
    me, col = lax.axis_index("ra"), lax.axis_index("cb")
    z, y = lax.div(me, ny), lax.rem(me, ny)
    core = lax.rem(col, 2)
    brow = ny * g

    def remote(src, dst, s, r, **where):
        return pltpu.make_async_remote_copy(
            src_ref=src, dst_ref=dst, send_sem=s, recv_sem=r, device_id=where, device_id_type=MESH
        )

    def rows(base, size):
        return pl.ds(pl.multiple_of(base, 16), size)

    def weights(layer, c):
        cols = pl.ds(pl.multiple_of(c * cw, 128), cw)
        gate, up, down = ((gate1, up1, down1), (gate2, up2, down2))[layer]
        k = layer * chunks + c
        return [
            pltpu.make_async_copy(gate.at[:, cols], both_v.at[k, :, pl.ds(0, cw)], w_sem.at[0, k]),
            pltpu.make_async_copy(up.at[:, cols], both_v.at[k, :, pl.ds(cw, cw)], w_sem.at[1, k]),
            pltpu.make_async_copy(down.at[cols, :], down_v.at[k], w_sem.at[2, k]),
        ]

    for layer in range(2):
        @pl.loop(0, chunks)
        def _(c):
            for copy in weights(layer, c):
                copy.start()

    barrier = pltpu.get_barrier_semaphore()
    for off in range(1, n):
        pl.semaphore_signal(barrier, inc=1, device_id={"ra": lax.rem(me + off, n)}, device_id_type=MESH)
    for off in range(1, nc):
        pl.semaphore_signal(barrier, inc=1, device_id={"cb": lax.rem(col + off, nc)}, device_id_type=MESH)

    def other_y(j):
        return z * ny + lax.rem(y + j, ny)

    def next_z(e):
        return lax.rem(z + (1 if e else nz - 1), nz) * ny + y

    def back_z(e):
        return lax.rem(z + (nz - 1 if e else 1), nz) * ny + y

    def place(e):
        return z if e else nz - 1 - z

    def y1_copy(s, j):
        return remote(
            y1_snd.at[s, j - 1], y1_rcv.at[s, ny - 1 - j], y1_s.at[j - 1, s], y1_r.at[ny - 1 - j, s], ra=other_y(j)
        )

    def ca_copy(s, e):
        return remote(ca_snd.at[s, e], ca_rcv.at[s, e], ca_s.at[e, s], ca_r.at[e, s], ra=next_z(e))

    def cb_copy(s, e):
        return remote(cb_snd.at[s, e], cb_rcv.at[s, e], cb_s.at[e, s], cb_r.at[e, s], ra=next_z(e))

    def y2_copy(s, j):
        return remote(
            y2_snd.at[s, j - 1], y2_rcv.at[s, ny - 1 - j], y2_s.at[j - 1, s], y2_r.at[ny - 1 - j, s], ra=other_y(j)
        )

    def h2_copy(s, base, j, owner):
        part = hid.at[s, rows(base + owner * g, g), :]
        return remote(part, part, h2_s.at[j - 1, s], h2_r.at[ny - 1 - j, s], ra=other_y(j))

    def ga_copy(s, e):
        part = hid.at[s, pl.ds(e * half + brow, g), :]
        return remote(part, part, ga_s.at[e, s], ga_r.at[e, s], ra=back_z(e))

    def gb_copy(s, e):
        part = hid.at[s, pl.ds(e * half, brow), :]
        return remote(part, part, gb_s.at[e, s], gb_r.at[e, s], ra=back_z(e))

    def h1_copy(s, e, j):
        return remote(
            hid.at[s, pl.ds(e * half + brow, g), :],
            hid.at[s, pl.ds(e * half + brow + (ny - j) * g, g), :],
            h1_s.at[e, j - 1, s], h1_r.at[e, ny - 1 - j, s], ra=other_y(j),
        )

    def ms_copy(layer, b, off):
        return remote(
            ms_snd.at[layer, b], ms_rcv.at[layer, b, n - 1 - off],
            ms_s.at[layer, b, off - 1], ms_r.at[layer, b, n - 1 - off], ra=lax.rem(me + off, n),
        )

    def br_copy(layer, b, off):
        return remote(
            br_snd.at[layer, b], br_rcv.at[layer, b, n - 1 - off],
            br_s.at[layer, b, off - 1], br_r.at[layer, b, n - 1 - off], ra=lax.rem(me + off, n),
        )

    def store_h(b, value):
        value = value.astype(BF16)
        for e in range(2):
            h_v[rows(b * tb + e * half, brow), :] = value[e * half : e * half + brow]
            for yy in range(ny):
                slot = lax.rem(yy - y + ny, ny)
                at = e * half + brow + yy * g
                h_v[rows(b * tb + e * half + brow + slot * g, g), :] = value[at : at + g]

    def squares(value):
        return spread(jnp.sum(value * value, axis=1, keepdims=True))

    def block_rows(b):
        return pl.ds(pl.multiple_of(b * tb, tb), tb)

    def start_blocks(b):
        value = tok[block_rows(b), :].astype(F32)
        mid[block_rows(b), :] = value
        ms_snd[0, b] = squares(value)

    for b in range(blocks):
        start_blocks(b)
    store_h(0, mid[0:tb, :] * pre1[...])

    pl.semaphore_wait(barrier, n - 1 + nc - 1)
    for b in range(blocks):
        for off in range(1, n):
            ms_copy(0, b, off).start()

    def factor_of(snd, rcv, copy, layer, b):
        for off in range(1, n):
            copy(layer, b, off).wait()
        total = snd[layer, b]
        for off in range(1, n):
            total = total + rcv[layer, b, off - 1]
        return column(lax.rsqrt(total / width + EPS))

    def prepare():
        for b in range(blocks):
            factor = factor_of(ms_snd, ms_rcv, ms_copy, 0, b)
            if b == 0:
                scale[block_rows(b), :] = factor
            else:
                scale[block_rows(b), :] = jnp.ones_like(factor)
                store_h(b, mid[block_rows(b), :] * factor[:, 0:1] * pre1[...])

    is_end = (z == 0) | (z == nz - 1)
    end_base = jnp.where(z == 0, 0, half)

    def item(u):
        later = u >= items + p.gap
        valid = ((u >= 0) & (u < items)) | (later & (u < 2 * items + p.gap))
        s = u - jnp.where(later, items + p.gap, 0)
        layer = jnp.where(later, 1, 0)
        b = lax.div(s, chunks)
        return valid, s, layer, b, s - b * chunks

    def tick(t, carry):
        @pl.when(t == chunks // 2)
        def _():
            prepare()

        valid, s, layer, b, c = item(t)

        @pl.when(valid)
        def _():
            for one in range(2):
                @pl.when((b == 0) & (layer == one))
                def _():
                    gate_copy, up_copy, _ = weights(one, c)
                    gate_copy.wait()
                    up_copy.wait()
            value = jnp.dot(h_v[block_rows(b), :], both_v[layer * chunks + c], preferred_element_type=F32)
            for e in range(2):
                at = e * half + brow
                acc[s, e * half : at + g, :] = value[e * half : at + g]
                for j in range(1, ny):
                    y1_snd[s, j - 1, e * g : (e + 1) * g, :] = value[at + j * g : at + (j + 1) * g].astype(BF16)
            for j in range(1, ny):
                y1_copy(s, j).start()

        valid1, s1, _, _, _ = item(t - LY)

        @pl.when(valid1)
        def _():
            for j in range(1, ny):
                y1_copy(s1, j).wait_recv()
            for e in range(2):
                mine = pl.ds(e * half + brow, g)
                total = acc[s1, mine, :]
                for j in range(1, ny):
                    total = total + y1_rcv[s1, j - 1, e * g : (e + 1) * g, :].astype(F32)
                acc[s1, mine, :] = total

        def chain(e, lag, snd, rcv, copy, base, size):
            at = place(e)
            ok, s, _, _, _ = item(t - lag - at * LZ)
            mine = pl.ds(e * half + base, size)

            @pl.when(ok & (at == 0))
            def _():
                snd[s, e] = acc[s, mine, :].astype(BF16)
                copy(s, e).start()

            @pl.when(ok & (at > 0) & (at < nz - 1))
            def _():
                copy(s, e).wait_recv()
                snd[s, e] = (acc[s, mine, :] + rcv[s, e].astype(F32)).astype(BF16)
                copy(s, e).start()

            @pl.when(ok & (at == nz - 1))
            def _():
                copy(s, e).wait_recv()
                acc[s, mine, :] += rcv[s, e].astype(F32)

        for e in range(2):
            chain(e, 0, cb_snd, cb_rcv, cb_copy, 0, brow)

        ok2, s2, _, _, _ = item(t - (nz - 1) * LZ)

        @pl.when(ok2 & is_end)
        def _():
            for j in range(1, ny):
                there = rows(end_base + lax.rem(y + j, ny) * g, g)
                y2_snd[s2, j - 1] = acc[s2, there, :].astype(BF16)
                y2_copy(s2, j).start()

        for e in range(2):
            chain(e, LY, ca_snd, ca_rcv, ca_copy, brow, g)

        ok3, s3, layer3, b3, c3 = item(t - p.act)

        @pl.when(ok3 & (c3 == 0) & (layer3 == 1))
        def _():
            scale[block_rows(b3), :] = factor_of(ms_snd, ms_rcv, ms_copy, 1, b3)

        @pl.when(ok3 & is_end)
        def _():
            def activate(value, row, to):
                factor = scale[rows(b3 * tb + row, g), 0:1]
                gv, uv = value[:, :cw] * factor, value[:, cw:] * factor
                hid[s3, rows(to, g), :] = (gv / (1.0 + jnp.exp(-gv)) * uv).astype(BF16)

            for j in range(1, ny):
                y2_copy(s3, j).wait_recv()
            own = end_base + y * g
            total = acc[s3, rows(own, g), :]
            for j in range(1, ny):
                total = total + y2_rcv[s3, j - 1].astype(F32)
            activate(total, own, own)
            for j in range(1, ny):
                h2_copy(s3, end_base, j, y).start()
            activate(acc[s3, rows(end_base + brow, g), :], end_base + brow + y * g, end_base + brow)
            for e in range(2):
                @pl.when(z == (nz - 1 if e else 0))
                def _():
                    ga_copy(s3, e).start()
                    for j in range(1, ny):
                        h1_copy(s3, e, j).start()

        for e in range(2):
            far = nz - 1 - place(e)
            ok, s, _, _, _ = item(t - p.act - far * LZ)

            @pl.when(ok & (far > 0))
            def _():
                ga_copy(s, e).wait_recv()
                for j in range(1, ny):
                    h1_copy(s, e, j).start()

            @pl.when(ok & (far > 0) & (far < nz - 1))
            def _():
                ga_copy(s, e).start()

        for e in range(2):
            far = nz - 1 - place(e)
            ok, s, _, _, _ = item(t - p.act - LY - far * LZ)

            @pl.when(ok & (far == 0))
            def _():
                for j in range(1, ny):
                    h2_copy(s, end_base, j, lax.rem(y + j, ny)).wait_recv()

            @pl.when(ok & (far > 0))
            def _():
                gb_copy(s, e).wait_recv()

            @pl.when(ok & (far < nz - 1))
            def _():
                gb_copy(s, e).start()

        ok4, s4, layer4, b4, c4 = item(t - p.down)

        @pl.when(ok4)
        def _():
            for e in range(2):
                for j in range(1, ny):
                    h1_copy(s4, e, j).wait_recv()
            for one in range(2):
                @pl.when((b4 == 0) & (layer4 == one))
                def _():
                    weights(one, c4)[2].wait()
            value = jnp.dot(hid[s4], down_v[layer4 * chunks + c4], preferred_element_type=F32)

            @pl.when(c4 == 0)
            def _():
                branch[block_rows(b4), :] = value

            @pl.when(c4 > 0)
            def _():
                branch[block_rows(b4), :] += value

            for j in range(1, ny):
                y1_copy(s4, j).wait_send()
                for e in range(2):
                    h1_copy(s4, e, j).wait_send()
            for e in range(2):
                @pl.when(place(e) < nz - 1)
                def _():
                    ca_copy(s4, e).wait_send()
                    cb_copy(s4, e).wait_send()

                @pl.when(place(e) > 0)
                def _():
                    ga_copy(s4, e).wait_send()
                    gb_copy(s4, e).wait_send()

            @pl.when(is_end)
            def _():
                for j in range(1, ny):
                    y2_copy(s4, j).wait_send()
                    h2_copy(s4, end_base, j, y).wait_send()

        def after(k):
            ok, _, layer, b, c = item(t - p.post[k])
            return ok & (c == chunks - 1), layer, b

        peer = col + 1 - 2 * core

        def d_copy(layer, b):
            away = branch.at[rows(b * tb + (1 - core) * half, half), :]
            return remote(away, d_rcv.at[layer, b], d_s.at[layer, b], d_r.at[layer, b], cb=peer)

        def x_copy(layer, b, k):
            bit = lax.rem(lax.div(col, 2 << k), 2)
            to = col + (1 - 2 * bit) * (2 << k)
            return remote(x_snd.at[layer, b, k], x_rcv.at[layer, b, k], x_s.at[layer, b, k], x_r.at[layer, b, k], cb=to)

        def t_copy(layer, b):
            part = tot.at[layer, b, rows(core * half, half), :]
            return remote(part, part, t_s.at[layer, b], t_r.at[layer, b], cb=peer)

        def whole(layer, b, total):
            base = core * half
            tot[layer, b, rows(base, brow), :] = total[:brow]
            for j in range(ny):
                to = base + brow + lax.rem(y + j, ny) * g
                tot[layer, b, rows(to, g), :] = total[brow + j * g : brow + (j + 1) * g]
            t_copy(layer, b).start()

        go, layer, b = after(0)

        @pl.when(go)
        def _():
            d_copy(layer, b).start()

        for k in range(p.kx + 1):
            go_k, layer_k, b_k = after(k + 1)

            @pl.when(go_k)
            def _():
                if k == 0:
                    d_copy(layer_k, b_k).wait()
                    total = branch[rows(b_k * tb + core * half, half), :] + d_rcv[layer_k, b_k]
                else:
                    x_copy(layer_k, b_k, k - 1).wait()
                    total = x_snd[layer_k, b_k, k - 1] + x_rcv[layer_k, b_k, k - 1]
                if k < p.kx:
                    x_snd[layer_k, b_k, k] = total
                    x_copy(layer_k, b_k, k).start()
                else:
                    whole(layer_k, b_k, total)

        go5, layer5, b5 = after(p.kx + 2)

        @pl.when(go5)
        def _():
            t_copy(layer5, b5).wait()
            br_snd[layer5, b5] = squares(tot[layer5, b5])
            for off in range(1, n):
                br_copy(layer5, b5, off).start()

        go6, layer6, b6 = after(p.kx + 3)

        for one in range(2):
            @pl.when(go6 & (layer6 == one))
            def _():
                factor = 0.5 * factor_of(br_snd, br_rcv, br_copy, one, b6)[:, 0:1]
                gain = (post1, post2)[one][...]
                middle = mid[block_rows(b6), :] + factor * tot[one, b6] * gain
                if one == 0:
                    mid[block_rows(b6), :] = middle
                    store_h(b6, middle * pre2[...])
                    ms_snd[1, b6] = squares(middle)
                    for off in range(1, n):
                        ms_copy(1, b6, off).start()
                else:
                    y_out[block_rows(b6), :] = middle.astype(BF16)

        return carry

    lax.fori_loop(0, p.ticks, tick, 0)


def solution(mesh):
    n, nc = mesh.shape["ra"], mesh.shape["cb"]

    def body(tokens, pre1, gate1, up1, down1, post1, pre2, gate2, up2, down2, post2):
        count, depth = tokens.shape
        p = Plan(n, nc, count, depth, gate1.shape[1])
        vmem = pl.BlockSpec(memory_space=pltpu.VMEM)
        hbm = pl.BlockSpec(memory_space=pl.ANY)
        dma = pltpu.SemaphoreType.DMA
        items, blocks, wide, ny = p.items, p.blocks, 2 * p.cw, p.ny
        scratch = [
            pltpu.VMEM((2 * p.chunks, depth, wide), BF16),
            pltpu.VMEM((2 * p.chunks, p.cw, depth), BF16),
            pltpu.VMEM((count, depth), BF16),
            pltpu.VMEM((count, depth), F32),
            pltpu.VMEM((items, p.tb, wide), F32),
            pltpu.VMEM((count, depth), F32),
            pltpu.VMEM((count, 128), F32),
            pltpu.VMEM((items, p.tb, p.cw), BF16),
        ]
        scratch += [pltpu.VMEM((items, ny - 1, 2 * p.g, wide), BF16)] * 2
        scratch += [pltpu.VMEM((items, 2, p.g, wide), BF16)] * 2
        scratch += [pltpu.VMEM((items, 2, ny * p.g, wide), BF16)] * 2
        scratch += [pltpu.VMEM((items, ny - 1, p.g, wide), BF16)] * 2
        scratch += [pltpu.VMEM((2, blocks, p.half, depth), F32)]
        scratch += [pltpu.VMEM((2, blocks, max(1, p.kx), p.half, depth), F32)] * 2
        scratch += [pltpu.VMEM((2, blocks, p.tb, depth), F32)]
        scratch += [pltpu.VMEM((2, blocks, 8, p.tb), F32), pltpu.VMEM((2, blocks, n - 1, 8, p.tb), F32)] * 2
        scratch += [dma((3, 2 * p.chunks))]
        scratch += [dma((ny - 1, items))] * 2 + [dma((2, items))] * 4 + [dma((ny - 1, items))] * 4
        scratch += [dma((2, items))] * 4 + [dma((2, ny - 1, items))] * 2
        scratch += [dma((2, blocks))] * 2 + [dma((2, blocks, max(1, p.kx)))] * 2 + [dma((2, blocks))] * 2
        scratch += [dma((2, blocks, n - 1))] * 4
        row = lambda gain: gain.reshape(1, depth)
        return pl.pallas_call(
            functools.partial(kernel, p, depth * n),
            out_shape=jax.ShapeDtypeStruct((count, depth), BF16),
            in_specs=[vmem] * 5 + [hbm] * 6,
            out_specs=vmem,
            scratch_shapes=scratch,
            compiler_params=pltpu.CompilerParams(
                collective_id=0, has_side_effects=True, vmem_limit_bytes=62 * 1024 * 1024
            ),
            name="both",
        )(tokens, row(pre1), row(post1), row(pre2), row(post2), gate1, up1, down1, gate2, up2, down2)

    in_specs = (
        P(None, "ra"), P("ra"), P("ra", "cb"), P("ra", "cb"), P("cb", "ra"), P("ra"),
        P("ra"), P("ra", "cb"), P("ra", "cb"), P("cb", "ra"), P("ra"),
    )
    return jax.shard_map(body, mesh=mesh, in_specs=in_specs, out_specs=P(None, "ra"), check_vma=False)
```

```python
import functools

import jax
import jax.numpy as jnp
from jax import lax
from jax.experimental import pallas as pl
from jax.experimental.pallas import tpu as pltpu
from jax.sharding import PartitionSpec as P

EPS = 1e-06
MESH = pl.DeviceIdType.MESH
F32 = jnp.float32
BF16 = jnp.bfloat16
LY, LZ, MY, MZ = 3, 3, 3, 3
POST = (2, 4, 2, 4)


def log2(n):
    return n.bit_length() - 1


def spread(col):
    return jnp.broadcast_to(col, (col.shape[0], 128)).T[0:1]


def column(row):
    return jnp.broadcast_to(row, (128, row.shape[1])).T


class Plan:
    def __init__(self, n, nc, tokens, depth, hidden):
        self.n, self.nc, self.tokens, self.depth = n, nc, tokens, depth
        self.ny = 1 << (log2(n) // 2)
        self.nz = n // self.ny
        self.kx = log2(nc) - 1
        self.tb = 64 * self.ny
        self.half, self.g = self.tb // 2, 16
        self.cw = 256 if hidden % 256 == 0 else 128
        self.chunks, self.blocks = hidden // self.cw, tokens // self.tb
        self.items = self.chunks * self.blocks
        self.act = (self.nz - 1) * LZ + LY
        self.down = self.act + MY + (self.nz - 1) * MZ
        steps = [0, POST[0]] + [POST[1]] * self.kx + [POST[2], POST[3]]
        self.post = [self.down + sum(steps[: i + 1]) for i in range(len(steps))]
        self.gap = max(0, self.chunks + self.post[-1] - self.items)
        self.ticks = 2 * self.items + self.gap + self.post[-1]


def kernel(p, width, *refs):
    (tok, pre1, post1, pre2, post2, gate1, up1, down1, gate2, up2, down2, y_out), refs = refs[:12], refs[12:]
    (both_v, down_v, h_v, mid, acc, branch, scale, hid), refs = refs[:8], refs[8:]
    (y1_snd, y1_rcv, ca_snd, ca_rcv, cb_snd, cb_rcv, y2_snd, y2_rcv), refs = refs[:8], refs[8:]
    (d_rcv, x_snd, x_rcv, tot, br_snd, br_rcv, ms_snd, ms_rcv), refs = refs[:8], refs[8:]
    (w_sem, y1_s, y1_r, ca_s, ca_r, cb_s, cb_r, y2_s, y2_r, h2_s, h2_r, ga_s, ga_r, gb_s, gb_r, h1_s, h1_r), refs = (
        refs[:17], refs[17:],
    )
    d_s, d_r, x_s, x_r, t_s, t_r, br_s, br_r, ms_s, ms_r = refs

    n, nc, ny, nz, tb, half, g, cw = p.n, p.nc, p.ny, p.nz, p.tb, p.half, p.g, p.cw
    chunks, blocks, items = p.chunks, p.blocks, p.items
    me, col = lax.axis_index("ra"), lax.axis_index("cb")
    z, y = lax.div(me, ny), lax.rem(me, ny)
    core = lax.rem(col, 2)
    brow = ny * g

    def remote(src, dst, s, r, **where):
        return pltpu.make_async_remote_copy(
            src_ref=src, dst_ref=dst, send_sem=s, recv_sem=r, device_id=where, device_id_type=MESH
        )

    def rows(base, size):
        return pl.ds(pl.multiple_of(base, 16), size)

    def weights(layer, c):
        cols = pl.ds(pl.multiple_of(c * cw, 128), cw)
        gate, up, down = ((gate1, up1, down1), (gate2, up2, down2))[layer]
        k = layer * chunks + c
        return [
            pltpu.make_async_copy(gate.at[:, cols], both_v.at[k, :, pl.ds(0, cw)], w_sem.at[0, k]),
            pltpu.make_async_copy(up.at[:, cols], both_v.at[k, :, pl.ds(cw, cw)], w_sem.at[1, k]),
            pltpu.make_async_copy(down.at[cols, :], down_v.at[k], w_sem.at[2, k]),
        ]

    def fetch(layer):
        @pl.loop(0, chunks)
        def _(c):
            for copy in weights(layer, c):
                copy.start()

    fetch(0)

    barrier = pltpu.get_barrier_semaphore()
    for off in range(1, n):
        pl.semaphore_signal(barrier, inc=1, device_id={"ra": lax.rem(me + off, n)}, device_id_type=MESH)
    for off in range(1, nc):
        pl.semaphore_signal(barrier, inc=1, device_id={"cb": lax.rem(col + off, nc)}, device_id_type=MESH)

    def other_y(j):
        return z * ny + lax.rem(y + j, ny)

    def next_z(e):
        return lax.rem(z + (1 if e else nz - 1), nz) * ny + y

    def back_z(e):
        return lax.rem(z + (nz - 1 if e else 1), nz) * ny + y

    def place(e):
        return z if e else nz - 1 - z

    def y1_copy(s, j):
        return remote(
            y1_snd.at[s, j - 1], y1_rcv.at[s, ny - 1 - j], y1_s.at[j - 1, s], y1_r.at[ny - 1 - j, s], ra=other_y(j)
        )

    def ca_copy(s, e):
        return remote(ca_snd.at[s, e], ca_rcv.at[s, e], ca_s.at[e, s], ca_r.at[e, s], ra=next_z(e))

    def cb_copy(s, e):
        return remote(cb_snd.at[s, e], cb_rcv.at[s, e], cb_s.at[e, s], cb_r.at[e, s], ra=next_z(e))

    def y2_copy(s, j):
        return remote(
            y2_snd.at[s, j - 1], y2_rcv.at[s, ny - 1 - j], y2_s.at[j - 1, s], y2_r.at[ny - 1 - j, s], ra=other_y(j)
        )

    def h2_copy(s, base, j, owner):
        part = hid.at[s, rows(base + owner * g, g), :]
        return remote(part, part, h2_s.at[j - 1, s], h2_r.at[ny - 1 - j, s], ra=other_y(j))

    def ga_copy(s, e):
        part = hid.at[s, pl.ds(e * half + brow, g), :]
        return remote(part, part, ga_s.at[e, s], ga_r.at[e, s], ra=back_z(e))

    def gb_copy(s, e):
        part = hid.at[s, pl.ds(e * half, brow), :]
        return remote(part, part, gb_s.at[e, s], gb_r.at[e, s], ra=back_z(e))

    def h1_copy(s, e, j):
        return remote(
            hid.at[s, pl.ds(e * half + brow, g), :],
            hid.at[s, pl.ds(e * half + brow + (ny - j) * g, g), :],
            h1_s.at[e, j - 1, s], h1_r.at[e, ny - 1 - j, s], ra=other_y(j),
        )

    def ms_copy(layer, b, off):
        return remote(
            ms_snd.at[layer, b], ms_rcv.at[layer, b, n - 1 - off],
            ms_s.at[layer, b, off - 1], ms_r.at[layer, b, n - 1 - off], ra=lax.rem(me + off, n),
        )

    def br_copy(layer, b, off):
        return remote(
            br_snd.at[layer, b], br_rcv.at[layer, b, n - 1 - off],
            br_s.at[layer, b, off - 1], br_r.at[layer, b, n - 1 - off], ra=lax.rem(me + off, n),
        )

    def store_h(b, value):
        value = value.astype(BF16)
        for e in range(2):
            h_v[rows(b * tb + e * half, brow), :] = value[e * half : e * half + brow]
            for yy in range(ny):
                slot = lax.rem(yy - y + ny, ny)
                at = e * half + brow + yy * g
                h_v[rows(b * tb + e * half + brow + slot * g, g), :] = value[at : at + g]

    def squares(value):
        return spread(jnp.sum(value * value, axis=1, keepdims=True))

    def block_rows(b):
        return pl.ds(pl.multiple_of(b * tb, tb), tb)

    def start_blocks(b):
        value = tok[block_rows(b), :].astype(F32)
        mid[block_rows(b), :] = value
        ms_snd[0, b] = squares(value)

    for b in range(blocks):
        start_blocks(b)
    store_h(0, mid[0:tb, :] * pre1[...])

    pl.semaphore_wait(barrier, n - 1 + nc - 1)
    for b in range(blocks):
        for off in range(1, n):
            ms_copy(0, b, off).start()

    def factor_of(snd, rcv, copy, layer, b):
        for off in range(1, n):
            copy(layer, b, off).wait()
        total = snd[layer, b]
        for off in range(1, n):
            total = total + rcv[layer, b, off - 1]
        return column(lax.rsqrt(total / width + EPS))

    def prepare():
        for b in range(blocks):
            factor = factor_of(ms_snd, ms_rcv, ms_copy, 0, b)
            if b == 0:
                scale[block_rows(b), :] = factor
            else:
                scale[block_rows(b), :] = jnp.ones_like(factor)
                store_h(b, mid[block_rows(b), :] * factor[:, 0:1] * pre1[...])

    is_end = (z == 0) | (z == nz - 1)
    end_base = jnp.where(z == 0, 0, half)

    def item(u):
        later = u >= items + p.gap
        valid = ((u >= 0) & (u < items)) | (later & (u < 2 * items + p.gap))
        s = u - jnp.where(later, items + p.gap, 0)
        layer = jnp.where(later, 1, 0)
        b = lax.div(s, chunks)
        return valid, s, layer, b, s - b * chunks

    def tick(t, carry):
        @pl.when(t == chunks // 2)
        def _():
            prepare()
            fetch(1)

        valid, s, layer, b, c = item(t)

        @pl.when(valid)
        def _():
            for one in range(2):
                @pl.when((b == 0) & (layer == one))
                def _():
                    gate_copy, up_copy, _ = weights(one, c)
                    gate_copy.wait()
                    up_copy.wait()
            value = jnp.dot(h_v[block_rows(b), :], both_v[layer * chunks + c], preferred_element_type=F32)
            for e in range(2):
                at = e * half + brow
                acc[s, e * half : at + g, :] = value[e * half : at + g]
                for j in range(1, ny):
                    y1_snd[s, j - 1, e * g : (e + 1) * g, :] = value[at + j * g : at + (j + 1) * g].astype(BF16)
            for j in range(1, ny):
                y1_copy(s, j).start()

        valid1, s1, _, _, _ = item(t - LY)

        @pl.when(valid1)
        def _():
            for j in range(1, ny):
                y1_copy(s1, j).wait_recv()
            for e in range(2):
                mine = pl.ds(e * half + brow, g)
                total = acc[s1, mine, :]
                for j in range(1, ny):
                    total = total + y1_rcv[s1, j - 1, e * g : (e + 1) * g, :].astype(F32)
                acc[s1, mine, :] = total

        def chain(e, lag, snd, rcv, copy, base, size):
            at = place(e)
            ok, s, _, _, _ = item(t - lag - at * LZ)
            mine = pl.ds(e * half + base, size)

            @pl.when(ok & (at == 0))
            def _():
                snd[s, e] = acc[s, mine, :].astype(BF16)
                copy(s, e).start()

            @pl.when(ok & (at > 0) & (at < nz - 1))
            def _():
                copy(s, e).wait_recv()
                snd[s, e] = (acc[s, mine, :] + rcv[s, e].astype(F32)).astype(BF16)
                copy(s, e).start()

            @pl.when(ok & (at == nz - 1))
            def _():
                copy(s, e).wait_recv()
                acc[s, mine, :] += rcv[s, e].astype(F32)

        for e in range(2):
            chain(e, 0, cb_snd, cb_rcv, cb_copy, 0, brow)

        ok2, s2, _, _, _ = item(t - (nz - 1) * LZ)

        @pl.when(ok2 & is_end)
        def _():
            for j in range(1, ny):
                there = rows(end_base + lax.rem(y + j, ny) * g, g)
                y2_snd[s2, j - 1] = acc[s2, there, :].astype(BF16)
                y2_copy(s2, j).start()

        for e in range(2):
            chain(e, LY, ca_snd, ca_rcv, ca_copy, brow, g)

        ok3, s3, layer3, b3, c3 = item(t - p.act)

        @pl.when(ok3 & (c3 == 0) & (layer3 == 1))
        def _():
            scale[block_rows(b3), :] = factor_of(ms_snd, ms_rcv, ms_copy, 1, b3)

        @pl.when(ok3 & is_end)
        def _():
            def activate(value, row, to):
                factor = scale[rows(b3 * tb + row, g), 0:1]
                gv, uv = value[:, :cw] * factor, value[:, cw:] * factor
                hid[s3, rows(to, g), :] = (gv / (1.0 + jnp.exp(-gv)) * uv).astype(BF16)

            for j in range(1, ny):
                y2_copy(s3, j).wait_recv()
            own = end_base + y * g
            total = acc[s3, rows(own, g), :]
            for j in range(1, ny):
                total = total + y2_rcv[s3, j - 1].astype(F32)
            activate(total, own, own)
            for j in range(1, ny):
                h2_copy(s3, end_base, j, y).start()
            activate(acc[s3, rows(end_base + brow, g), :], end_base + brow + y * g, end_base + brow)
            for e in range(2):
                @pl.when(z == (nz - 1 if e else 0))
                def _():
                    ga_copy(s3, e).start()
                    for j in range(1, ny):
                        h1_copy(s3, e, j).start()

        for e in range(2):
            far = nz - 1 - place(e)
            ok, s, _, _, _ = item(t - p.act - far * MZ)

            @pl.when(ok & (far > 0))
            def _():
                ga_copy(s, e).wait_recv()
                for j in range(1, ny):
                    h1_copy(s, e, j).start()

            @pl.when(ok & (far > 0) & (far < nz - 1))
            def _():
                ga_copy(s, e).start()

        for e in range(2):
            far = nz - 1 - place(e)
            ok, s, _, _, _ = item(t - p.act - MY - far * MZ)

            @pl.when(ok & (far == 0))
            def _():
                for j in range(1, ny):
                    h2_copy(s, end_base, j, lax.rem(y + j, ny)).wait_recv()

            @pl.when(ok & (far > 0))
            def _():
                gb_copy(s, e).wait_recv()

            @pl.when(ok & (far < nz - 1))
            def _():
                gb_copy(s, e).start()

        ok4, s4, layer4, b4, c4 = item(t - p.down)

        @pl.when(ok4)
        def _():
            for e in range(2):
                for j in range(1, ny):
                    h1_copy(s4, e, j).wait_recv()
            for one in range(2):
                @pl.when((b4 == 0) & (layer4 == one))
                def _():
                    weights(one, c4)[2].wait()
            value = jnp.dot(hid[s4], down_v[layer4 * chunks + c4], preferred_element_type=F32)

            @pl.when(c4 == 0)
            def _():
                branch[block_rows(b4), :] = value

            @pl.when(c4 > 0)
            def _():
                branch[block_rows(b4), :] += value

            for j in range(1, ny):
                y1_copy(s4, j).wait_send()
                for e in range(2):
                    h1_copy(s4, e, j).wait_send()
            for e in range(2):
                @pl.when(place(e) < nz - 1)
                def _():
                    ca_copy(s4, e).wait_send()
                    cb_copy(s4, e).wait_send()

                @pl.when(place(e) > 0)
                def _():
                    ga_copy(s4, e).wait_send()
                    gb_copy(s4, e).wait_send()

            @pl.when(is_end)
            def _():
                for j in range(1, ny):
                    y2_copy(s4, j).wait_send()
                    h2_copy(s4, end_base, j, y).wait_send()

        def after(k):
            ok, _, layer, b, c = item(t - p.post[k])
            return ok & (c == chunks - 1), layer, b

        peer = col + 1 - 2 * core

        def d_copy(layer, b):
            away = branch.at[rows(b * tb + (1 - core) * half, half), :]
            return remote(away, d_rcv.at[layer, b], d_s.at[layer, b], d_r.at[layer, b], cb=peer)

        def x_copy(layer, b, k):
            bit = lax.rem(lax.div(col, 2 << k), 2)
            to = col + (1 - 2 * bit) * (2 << k)
            return remote(x_snd.at[layer, b, k], x_rcv.at[layer, b, k], x_s.at[layer, b, k], x_r.at[layer, b, k], cb=to)

        def t_copy(layer, b):
            part = tot.at[layer, b, rows(core * half, half), :]
            return remote(part, part, t_s.at[layer, b], t_r.at[layer, b], cb=peer)

        def whole(layer, b, total):
            base = core * half
            tot[layer, b, rows(base, brow), :] = total[:brow]
            for j in range(ny):
                to = base + brow + lax.rem(y + j, ny) * g
                tot[layer, b, rows(to, g), :] = total[brow + j * g : brow + (j + 1) * g]
            t_copy(layer, b).start()

        go, layer, b = after(0)

        @pl.when(go)
        def _():
            d_copy(layer, b).start()

        for k in range(p.kx + 1):
            go_k, layer_k, b_k = after(k + 1)

            @pl.when(go_k)
            def _():
                if k == 0:
                    d_copy(layer_k, b_k).wait()
                    total = branch[rows(b_k * tb + core * half, half), :] + d_rcv[layer_k, b_k]
                else:
                    x_copy(layer_k, b_k, k - 1).wait()
                    total = x_snd[layer_k, b_k, k - 1] + x_rcv[layer_k, b_k, k - 1]
                if k < p.kx:
                    x_snd[layer_k, b_k, k] = total
                    x_copy(layer_k, b_k, k).start()
                else:
                    whole(layer_k, b_k, total)

        go5, layer5, b5 = after(p.kx + 2)

        @pl.when(go5)
        def _():
            t_copy(layer5, b5).wait()
            br_snd[layer5, b5] = squares(tot[layer5, b5])
            for off in range(1, n):
                br_copy(layer5, b5, off).start()

        go6, layer6, b6 = after(p.kx + 3)

        for one in range(2):
            @pl.when(go6 & (layer6 == one))
            def _():
                factor = 0.5 * factor_of(br_snd, br_rcv, br_copy, one, b6)[:, 0:1]
                gain = (post1, post2)[one][...]
                middle = mid[block_rows(b6), :] + factor * tot[one, b6] * gain
                if one == 0:
                    mid[block_rows(b6), :] = middle
                    store_h(b6, middle * pre2[...])
                    ms_snd[1, b6] = squares(middle)
                    for off in range(1, n):
                        ms_copy(1, b6, off).start()
                else:
                    y_out[block_rows(b6), :] = middle.astype(BF16)

        return carry

    lax.fori_loop(0, p.ticks, tick, 0)


def solution(mesh):
    n, nc = mesh.shape["ra"], mesh.shape["cb"]

    def body(tokens, pre1, gate1, up1, down1, post1, pre2, gate2, up2, down2, post2):
        count, depth = tokens.shape
        p = Plan(n, nc, count, depth, gate1.shape[1])
        vmem = pl.BlockSpec(memory_space=pltpu.VMEM)
        hbm = pl.BlockSpec(memory_space=pl.ANY)
        dma = pltpu.SemaphoreType.DMA
        items, blocks, wide, ny = p.items, p.blocks, 2 * p.cw, p.ny
        scratch = [
            pltpu.VMEM((2 * p.chunks, depth, wide), BF16),
            pltpu.VMEM((2 * p.chunks, p.cw, depth), BF16),
            pltpu.VMEM((count, depth), BF16),
            pltpu.VMEM((count, depth), F32),
            pltpu.VMEM((items, p.tb, wide), F32),
            pltpu.VMEM((count, depth), F32),
            pltpu.VMEM((count, 128), F32),
            pltpu.VMEM((items, p.tb, p.cw), BF16),
        ]
        scratch += [pltpu.VMEM((items, ny - 1, 2 * p.g, wide), BF16)] * 2
        scratch += [pltpu.VMEM((items, 2, p.g, wide), BF16)] * 2
        scratch += [pltpu.VMEM((items, 2, ny * p.g, wide), BF16)] * 2
        scratch += [pltpu.VMEM((items, ny - 1, p.g, wide), BF16)] * 2
        scratch += [pltpu.VMEM((2, blocks, p.half, depth), F32)]
        scratch += [pltpu.VMEM((2, blocks, max(1, p.kx), p.half, depth), F32)] * 2
        scratch += [pltpu.VMEM((2, blocks, p.tb, depth), F32)]
        scratch += [pltpu.VMEM((2, blocks, 1, p.tb), F32), pltpu.VMEM((2, blocks, n - 1, 1, p.tb), F32)] * 2
        scratch += [dma((3, 2 * p.chunks))]
        scratch += [dma((ny - 1, items))] * 2 + [dma((2, items))] * 4 + [dma((ny - 1, items))] * 4
        scratch += [dma((2, items))] * 4 + [dma((2, ny - 1, items))] * 2
        scratch += [dma((2, blocks))] * 2 + [dma((2, blocks, max(1, p.kx)))] * 2 + [dma((2, blocks))] * 2
        scratch += [dma((2, blocks, n - 1))] * 4
        row = lambda gain: gain.reshape(1, depth)
        return pl.pallas_call(
            functools.partial(kernel, p, depth * n),
            out_shape=jax.ShapeDtypeStruct((count, depth), BF16),
            in_specs=[vmem] * 5 + [hbm] * 6,
            out_specs=vmem,
            scratch_shapes=scratch,
            compiler_params=pltpu.CompilerParams(
                collective_id=0, has_side_effects=True, vmem_limit_bytes=62 * 1024 * 1024
            ),
            name="both",
        )(tokens, row(pre1), row(post1), row(pre2), row(post2), gate1, up1, down1, gate2, up2, down2)

    in_specs = (
        P(None, "ra"), P("ra"), P("ra", "cb"), P("ra", "cb"), P("cb", "ra"), P("ra"),
        P("ra"), P("ra", "cb"), P("ra", "cb"), P("cb", "ra"), P("ra"),
    )
    return jax.shard_map(body, mesh=mesh, in_specs=in_specs, out_specs=P(None, "ra"), check_vma=False)
```

```python
import functools

import jax
import jax.numpy as jnp
from jax import lax
from jax.experimental import pallas as pl
from jax.experimental.pallas import tpu as pltpu
from jax.sharding import PartitionSpec as P

EPS = 1e-06
MESH = pl.DeviceIdType.MESH
F32 = jnp.float32
BF16 = jnp.bfloat16
LY, LZ, MY, MZ = 3, 3, 3, 3
POST = (2, 3, 4)


def log2(n):
    return n.bit_length() - 1


def spread(col):
    return jnp.broadcast_to(col, (col.shape[0], 128)).T[0:1]


def column(row):
    return jnp.broadcast_to(row, (128, row.shape[1])).T


class Plan:
    def __init__(self, n, nc, tokens, depth, hidden):
        self.n, self.nc, self.tokens, self.depth = n, nc, tokens, depth
        self.ny = 1 << (log2(n) // 2)
        self.nz = n // self.ny
        self.kx = log2(nc) - 1
        self.tb = 64 * self.ny
        self.half, self.g = self.tb // 2, 16
        self.lanes = max(self.half, 128)
        self.cw = 256 if hidden % 256 == 0 else 128
        self.chunks, self.blocks = hidden // self.cw, tokens // self.tb
        self.items = self.chunks * self.blocks
        self.act = (self.nz - 1) * LZ + LY
        self.down = self.act + MY + (self.nz - 1) * MZ
        steps = [0, POST[0]] + [POST[1]] * self.kx + [POST[2]]
        self.post = [self.down + sum(steps[: i + 1]) for i in range(len(steps))]
        self.gap = max(0, self.chunks + self.post[-1] - self.items)
        self.ticks = 2 * self.items + self.gap + self.post[-1]
        self.ring = self.items + self.gap + max(LY, MY)


def kernel(p, width, *refs):
    (tok_hbm, pre1, post1, pre2, post2, gate1, up1, down1, gate2, up2, down2, y_hbm), refs = refs[:12], refs[12:]
    (both_v, down_v, h_v, mid, acc, branch, scale, hid), refs = refs[:8], refs[8:]
    (yr_snd, yr_rcv, zr_snd, zr_rcv, ya_snd, ya_rcv, za), refs = refs[:7], refs[7:]
    (d_rcv, x_snd, x_rcv, tot, br_snd, br_rcv, ms_snd, ms_rcv), refs = refs[:8], refs[8:]
    (w_sem, yr_s, yr_r, zr_s, zr_r, ya_s, ya_r, za_s, za_r), refs = refs[:9], refs[9:]
    d_s, d_r, x_s, x_r, t_s, t_r, br_s, br_r, ms_s, ms_r, fac, tok, y_out, io_s = refs

    n, nc, ny, nz, tb, half, g, cw = p.n, p.nc, p.ny, p.nz, p.tb, p.half, p.g, p.cw
    chunks, blocks, items = p.chunks, p.blocks, p.items
    me, col = lax.axis_index("ra"), lax.axis_index("cb")
    z, y = lax.div(me, ny), lax.rem(me, ny)
    core = lax.rem(col, 2)
    brow = ny * g

    def remote(src, dst, s, r, **where):
        return pltpu.make_async_remote_copy(
            src_ref=src, dst_ref=dst, send_sem=s, recv_sem=r, device_id=where, device_id_type=MESH
        )

    def rows(base, size):
        return pl.ds(pl.multiple_of(base, 16), size)

    def weights(layer, c):
        cols = pl.ds(pl.multiple_of(c * cw, 128), cw)
        gate, up, down = ((gate1, up1, down1), (gate2, up2, down2))[layer]
        k = layer * chunks + c
        return [
            pltpu.make_async_copy(gate.at[:, cols], both_v.at[k, :, pl.ds(0, cw)], w_sem.at[0, k]),
            pltpu.make_async_copy(up.at[:, cols], both_v.at[k, :, pl.ds(cw, cw)], w_sem.at[1, k]),
            pltpu.make_async_copy(down.at[cols, :], down_v.at[k], w_sem.at[2, k]),
        ]

    def fetch(layer, start):
        @pl.loop(start, chunks)
        def _(c):
            for copy in weights(layer, c):
                copy.start()

    tok_copy = pltpu.make_async_copy(tok_hbm, tok, io_s.at[0])
    tok_copy.start()
    for copy in weights(0, 0):
        copy.start()
    barrier = pltpu.get_barrier_semaphore()
    for off in range(1, n):
        pl.semaphore_signal(barrier, inc=1, device_id={"ra": lax.rem(me + off, n)}, device_id_type=MESH)
    for off in range(1, nc):
        pl.semaphore_signal(barrier, inc=1, device_id={"cb": lax.rem(col + off, nc)}, device_id_type=MESH)

    fetch(0, 1)

    def other_y(j):
        return z * ny + lax.rem(y + j, ny)

    def next_z(e):
        return lax.rem(z + (1 if e else nz - 1), nz) * ny + y

    def back_z(e):
        return lax.rem(z + (nz - 1 if e else 1), nz) * ny + y

    def place(e):
        return z if e else nz - 1 - z

    def yr_copy(slot, j, part):
        return remote(
            yr_snd.at[slot, j - 1, pl.ds(*part), :], yr_rcv.at[slot, ny - 1 - j, pl.ds(*part), :],
            yr_s.at[j - 1, slot], yr_r.at[ny - 1 - j, slot], ra=other_y(j),
        )

    def ya_copy(slot, j, part):
        return remote(
            ya_snd.at[slot, pl.ds(*part), :], ya_rcv.at[slot, ny - 1 - j, pl.ds(*part), :],
            ya_s.at[j - 1, slot], ya_r.at[ny - 1 - j, slot], ra=other_y(j),
        )

    def zr_copy(slot, e):
        return remote(zr_snd.at[slot, e], zr_rcv.at[slot, e], zr_s.at[e, slot], zr_r.at[e, slot], ra=next_z(e))

    def za_copy(slot, e):
        return remote(za.at[slot, e], za.at[slot, e], za_s.at[e, slot], za_r.at[e, slot], ra=back_z(e))

    def by_part(one, two, act):
        for ok, part in ((one & two, (0, 3 * g)), (one & ~two, (0, 2 * g)), (two & ~one, (2 * g, g))):
            @pl.when(ok)
            def _():
                for j in range(1, ny):
                    act(j, part)

    def ms_copy(layer, b, off):
        return remote(
            ms_snd.at[layer, b], ms_rcv.at[layer, b, n - 1 - off],
            ms_s.at[layer, b, off - 1], ms_r.at[layer, b, n - 1 - off], ra=lax.rem(me + off, n),
        )

    def br_copy(layer, b, off, across):
        start = n - 1 if across else -1
        to = start + (n - off) % n
        where = {"cb": col + 1 - 2 * core} if across else {}
        return remote(
            br_snd.at[layer, b], br_rcv.at[layer, b, to],
            br_s.at[layer, b, start + off], br_r.at[layer, b, to], ra=lax.rem(me + off, n), **where,
        )

    br_all = [(off, False) for off in range(1, n)] + [(off, True) for off in range(n)]

    def store_h(b, value):
        value = value.astype(BF16)
        for e in range(2):
            h_v[rows(b * tb + e * half, brow), :] = value[e * half : e * half + brow]
            for yy in range(ny):
                slot = lax.rem(yy - y + ny, ny)
                at = e * half + brow + yy * g
                h_v[rows(b * tb + e * half + brow + slot * g, g), :] = value[at : at + g]

    def squares(value):
        return spread(jnp.sum(value * value, axis=1, keepdims=True))

    def block_rows(b):
        return pl.ds(pl.multiple_of(b * tb, tb), tb)

    def start_blocks(b):
        value = tok[block_rows(b), :].astype(F32)
        mid[block_rows(b), :] = value
        ms_snd[0, b] = squares(value)

    tok_copy.wait()
    for b in range(blocks):
        start_blocks(b)
    store_h(0, mid[0:tb, :] * pre1[...])

    pl.semaphore_wait(barrier, n - 1 + nc - 1)

    def factor_of(layer, b):
        for off in range(1, n):
            ms_copy(layer, b, off).wait()
        total = ms_snd[layer, b]
        for off in range(1, n):
            total = total + ms_rcv[layer, b, off - 1]
        return column(lax.rsqrt(total / width + EPS))

    def prepare():
        for b in range(blocks):
            factor = factor_of(0, b)
            if b == 0:
                scale[block_rows(b), :] = factor
            else:
                scale[block_rows(b), :] = jnp.ones_like(factor)
                store_h(b, mid[block_rows(b), :] * factor[:, 0:1] * pre1[...])

    is_end = (z == 0) | (z == nz - 1)
    end = jnp.where(z == 0, 0, 1)
    last = nz - 1

    def item(u):
        later = u >= items + p.gap
        valid = ((u >= 0) & (u < items)) | (later & (u < 2 * items + p.gap))
        s = u - jnp.where(later, items + p.gap, 0)
        layer = jnp.where(later, 1, 0)
        b = lax.div(s, chunks)
        return valid, s, layer, b, s - b * chunks

    def y_copy(b):
        return pltpu.make_async_copy(y_out.at[block_rows(b), :], y_hbm.at[block_rows(b), :], io_s.at[1 + b])

    def slot_of(v):
        return lax.rem(jnp.maximum(v, 0), p.ring)

    def valid(u):
        return item(u)[0]

    def tick(t, carry):
        x = t - p.act
        y_slot, y_old = slot_of(t), slot_of(t - LY)
        g_slot, g_old = slot_of(x), slot_of(x - MY)

        @pl.when(t == chunks // 2)
        def _():
            prepare()
            fetch(1, 0)

        ok, s, layer, b, c = item(t)

        @pl.when(ok)
        def _():
            for one in range(2):
                @pl.when((b == 0) & (layer == one))
                def _():
                    gate_copy, up_copy, _ = weights(one, c)
                    gate_copy.wait()
                    up_copy.wait()
            value = jnp.dot(h_v[block_rows(b), :], both_v[layer * chunks + c], preferred_element_type=F32)
            for e in range(2):
                at = e * half + brow
                acc[s, e * half : at + g, :] = value[e * half : at + g]
                for j in range(1, ny):
                    yr_snd[y_slot, j - 1, e * g : (e + 1) * g, :] = value[at + j * g : at + (j + 1) * g].astype(BF16)

        by_part(
            valid(t - LY), is_end & valid(t - LY - last * LZ), lambda j, part: yr_copy(y_old, j, part).wait()
        )
        ok1, s1, _, _, _ = item(t - LY)

        @pl.when(ok1)
        def _():
            for e in range(2):
                mine = pl.ds(e * half + brow, g)
                total = acc[s1, mine, :]
                for j in range(1, ny):
                    total = total + yr_rcv[y_old, j - 1, e * g : (e + 1) * g, :].astype(F32)
                acc[s1, mine, :] = total

        for e in range(2):
            at = place(e)
            v = t - at * LZ
            now, old = slot_of(v), slot_of(v - LZ)
            ok_b, s_b, _, _, _ = item(v)
            ok_a, s_a, _, _, _ = item(v - LY)

            @pl.when((ok_b | ok_a) & (at > 0))
            def _():
                zr_copy(now, e).wait_recv()

            for ok_i, s_i, base, size in ((ok_b, s_b, 0, brow), (ok_a, s_a, brow, g)):
                mine, part = pl.ds(e * half + base, size), pl.ds(base, size)

                @pl.when(ok_i & (at == 0))
                def _():
                    zr_snd[now, e, part, :] = acc[s_i, mine, :].astype(BF16)

                @pl.when(ok_i & (at > 0) & (at < last))
                def _():
                    zr_snd[now, e, part, :] = (
                        acc[s_i, mine, :] + zr_rcv[now, e, part, :].astype(F32)
                    ).astype(BF16)

                @pl.when(ok_i & (at == last))
                def _():
                    acc[s_i, mine, :] += zr_rcv[now, e, part, :].astype(F32)

            @pl.when((ok_b | ok_a) & (at < last))
            def _():
                zr_copy(now, e).start()

            @pl.when((valid(v - LZ) | valid(v - LZ - LY)) & (at < last))
            def _():
                zr_copy(old, e).wait_send()

        ok2, s2, _, _, _ = item(t - last * LZ)

        @pl.when(ok2 & is_end)
        def _():
            for j in range(1, ny):
                there = rows(end * half + lax.rem(y + j, ny) * g, g)
                yr_snd[y_slot, j - 1, 2 * g :, :] = acc[s2, there, :].astype(BF16)

        by_part(ok, ok2 & is_end, lambda j, part: yr_copy(y_slot, j, part).start())

        ok3, s3, layer3, b3, c3 = item(x)

        @pl.when(ok3 & (c3 == 0) & (layer3 == 1))
        def _():
            scale[block_rows(b3), :] = factor_of(1, b3)

        @pl.when(ok3 & is_end)
        def _():
            def activate(value, row):
                factor = scale[rows(b3 * tb + row, g), 0:1]
                gv, uv = value[:, :cw] * factor, value[:, cw:] * factor
                return (gv / (1.0 + jnp.exp(-gv)) * uv).astype(BF16)

            own = end * half + y * g
            total = acc[s3, rows(own, g), :]
            for j in range(1, ny):
                total = total + yr_rcv[y_old, j - 1, 2 * g :, :].astype(F32)
            value = activate(total, own)
            hid[s3, rows(own, g), :] = value
            ya_snd[g_slot, 2 * g :, :] = value
            own = rows(end * half + brow, g)
            hid[s3, own, :] = activate(acc[s3, own, :], end * half + brow + y * g)

        by_part(
            valid(x - MY - last * MZ), is_end & valid(x - MY), lambda j, part: ya_copy(g_old, j, part).wait()
        )
        ok4, s4, layer4, b4, c4 = item(t - p.down)
        ok5, s5, _, _, _ = item(x - MY)

        @pl.when(ok4)
        def _():
            for e in range(2):
                for j in range(1, ny):
                    to = e * half + brow + j * g
                    hid[s4, to : to + g, :] = ya_rcv[g_old, j - 1, e * g : (e + 1) * g, :]

        @pl.when(ok5 & is_end)
        def _():
            for j in range(1, ny):
                hid[s5, rows(end * half + lax.rem(y + j, ny) * g, g), :] = ya_rcv[g_old, j - 1, 2 * g :, :]

        for e in range(2):
            far = last - place(e)
            w = x - far * MZ
            now, old = slot_of(w), slot_of(w - MZ)
            ok_a, s_a, _, _, _ = item(w)
            ok_b, s_b, _, _, _ = item(w - MY)

            @pl.when((ok_a | ok_b) & (far > 0))
            def _():
                za_copy(now, e).wait_recv()

            for ok_i, s_i, base, size in ((ok_b, s_b, 0, brow), (ok_a, s_a, brow, g)):
                mine, part = pl.ds(e * half + base, size), pl.ds(base, size)

                @pl.when(ok_i & (far == 0))
                def _():
                    za[now, e, part, :] = hid[s_i, mine, :]

            @pl.when((ok_a | ok_b) & (far < last))
            def _():
                za_copy(now, e).start()

            for ok_i, s_i, base, size in ((ok_b, s_b, 0, brow), (ok_a, s_a, brow, g)):
                mine, part = pl.ds(e * half + base, size), pl.ds(base, size)

                @pl.when(ok_i & (far > 0))
                def _():
                    hid[s_i, mine, :] = za[now, e, part, :]

            @pl.when((valid(w - MZ) | valid(w - MZ - MY)) & (far < last))
            def _():
                za_copy(old, e).wait_send()

        ok6, s6, _, _, _ = item(x - last * MZ)

        @pl.when(ok6)
        def _():
            for e in range(2):
                at = e * half + brow
                ya_snd[g_slot, e * g : (e + 1) * g, :] = hid[s6, at : at + g, :]

        by_part(ok6, ok3 & is_end, lambda j, part: ya_copy(g_slot, j, part).start())

        @pl.when(ok4)
        def _():
            for one in range(2):
                @pl.when((b4 == 0) & (layer4 == one))
                def _():
                    weights(one, c4)[2].wait()
            value = jnp.dot(hid[s4], down_v[layer4 * chunks + c4], preferred_element_type=F32)

            @pl.when(c4 == 0)
            def _():
                branch[block_rows(b4), :] = value

            @pl.when(c4 > 0)
            def _():
                branch[block_rows(b4), :] += value

        @pl.when(t == 0)
        def _():
            for b in range(blocks):
                for off in range(1, n):
                    ms_copy(0, b, off).start()

        def after(k):
            ok, _, layer, b, c = item(t - p.post[k])
            return ok & (c == chunks - 1), layer, b

        peer = col + 1 - 2 * core

        def d_copy(layer, b):
            away = branch.at[rows(b * tb + (1 - core) * half, half), :]
            return remote(away, d_rcv.at[layer, b], d_s.at[layer, b], d_r.at[layer, b], cb=peer)

        def x_copy(layer, b, k):
            bit = lax.rem(lax.div(col, 2 << k), 2)
            to = col + (1 - 2 * bit) * (2 << k)
            return remote(x_snd.at[layer, b, k], x_rcv.at[layer, b, k], x_s.at[layer, b, k], x_r.at[layer, b, k], cb=to)

        def t_copy(layer, b):
            part = tot.at[layer, b, rows(core * half, half), :]
            return remote(part, part, t_s.at[layer, b], t_r.at[layer, b], cb=peer)

        def whole(layer, b, total):
            base = core * half
            tot[layer, b, rows(base, brow), :] = total[:brow]
            for j in range(ny):
                to = base + brow + lax.rem(y + j, ny) * g
                tot[layer, b, rows(to, g), :] = total[brow + j * g : brow + (j + 1) * g]
            t_copy(layer, b).start()
            value = tot[layer, b, rows(base, half), :]
            sums = jnp.sum(value * value, axis=1, keepdims=True)
            if p.lanes > half:
                sums = jnp.concatenate([sums, jnp.zeros((p.lanes - half, 1), F32)], axis=0)
            br_snd[layer, b] = spread(sums)
            for off, across in br_all:
                br_copy(layer, b, off, across).start()

        go, layer, b = after(0)

        @pl.when(go)
        def _():
            d_copy(layer, b).start()

        for k in range(p.kx + 1):
            go_k, layer_k, b_k = after(k + 1)

            @pl.when(go_k)
            def _():
                if k == 0:
                    d_copy(layer_k, b_k).wait()
                    total = branch[rows(b_k * tb + core * half, half), :] + d_rcv[layer_k, b_k]
                else:
                    x_copy(layer_k, b_k, k - 1).wait()
                    total = x_snd[layer_k, b_k, k - 1].astype(F32) + x_rcv[layer_k, b_k, k - 1].astype(F32)
                if k < p.kx:
                    x_snd[layer_k, b_k, k] = total.astype(BF16)
                    x_copy(layer_k, b_k, k).start()
                else:
                    whole(layer_k, b_k, total)

        go6, layer6, b6 = after(p.kx + 2)

        for one in range(2):
            @pl.when(go6 & (layer6 == one))
            def _():
                t_copy(one, b6).wait()
                for off, across in br_all:
                    br_copy(one, b6, off, across).wait()
                own, other = br_snd[one, b6], br_rcv[one, b6, n - 1]
                for off in range(1, n):
                    own = own + br_rcv[one, b6, off - 1]
                    other = other + br_rcv[one, b6, n - 1 + off]
                for base, total in ((core * half, own), ((1 - core) * half, other)):
                    fac[rows(base, half), :] = column(0.5 * lax.rsqrt(total / width + EPS))[:half]
                factor = fac[:, 0:1]
                gain = (post1, post2)[one][...]
                middle = mid[block_rows(b6), :] + factor * tot[one, b6] * gain
                if one == 0:
                    mid[block_rows(b6), :] = middle
                    store_h(b6, middle * pre2[...])
                    ms_snd[1, b6] = squares(middle)
                    for off in range(1, n):
                        ms_copy(1, b6, off).start()
                else:
                    y_out[block_rows(b6), :] = middle.astype(BF16)
                    y_copy(b6).start()

        return carry

    lax.fori_loop(0, p.ticks, tick, 0)
    for b in range(blocks):
        y_copy(b).wait()


def solution(mesh):
    n, nc = mesh.shape["ra"], mesh.shape["cb"]

    def body(tokens, pre1, gate1, up1, down1, post1, pre2, gate2, up2, down2, post2):
        count, depth = tokens.shape
        p = Plan(n, nc, count, depth, gate1.shape[1])
        vmem = pl.BlockSpec(memory_space=pltpu.VMEM)
        hbm = pl.BlockSpec(memory_space=pl.ANY)
        dma = pltpu.SemaphoreType.DMA
        items, blocks, wide, ny = p.items, p.blocks, 2 * p.cw, p.ny
        scratch = [
            pltpu.VMEM((2 * p.chunks, depth, wide), BF16),
            pltpu.VMEM((2 * p.chunks, p.cw, depth), BF16),
            pltpu.VMEM((count, depth), BF16),
            pltpu.VMEM((count, depth), F32),
            pltpu.VMEM((items, p.tb, wide), F32),
            pltpu.VMEM((count, depth), F32),
            pltpu.VMEM((count, 128), F32),
            pltpu.VMEM((items, p.tb, p.cw), BF16),
        ]
        ring, many = p.ring, (ny + 1) * p.g
        scratch += [pltpu.VMEM((ring, ny - 1, 3 * p.g, wide), BF16)] * 2
        scratch += [pltpu.VMEM((ring, 2, many, wide), BF16)] * 2
        scratch += [pltpu.VMEM((ring, 3 * p.g, p.cw), BF16), pltpu.VMEM((ring, ny - 1, 3 * p.g, p.cw), BF16)]
        scratch += [pltpu.VMEM((ring, 2, many, p.cw), BF16)]
        scratch += [pltpu.VMEM((2, blocks, p.half, depth), F32)]
        scratch += [pltpu.VMEM((2, blocks, max(1, p.kx), p.half, depth), BF16)] * 2
        scratch += [pltpu.VMEM((2, blocks, p.tb, depth), F32)]
        scratch += [pltpu.VMEM((2, blocks, 1, p.lanes), F32), pltpu.VMEM((2, blocks, 2 * n - 1, 1, p.lanes), F32)]
        scratch += [pltpu.VMEM((2, blocks, 1, p.tb), F32), pltpu.VMEM((2, blocks, n - 1, 1, p.tb), F32)]
        scratch += [dma((3, 2 * p.chunks))]
        scratch += ([dma((ny - 1, ring))] * 2 + [dma((2, ring))] * 2) * 2
        scratch += [dma((2, blocks))] * 2 + [dma((2, blocks, max(1, p.kx)))] * 2 + [dma((2, blocks))] * 2
        scratch += [dma((2, blocks, 2 * n - 1))] * 2 + [dma((2, blocks, n - 1))] * 2
        scratch += [pltpu.VMEM((p.tb, 128), F32)] + [pltpu.VMEM((count, depth), BF16)] * 2 + [dma((1 + blocks,))]
        row = lambda gain: gain.reshape(1, depth)
        return pl.pallas_call(
            functools.partial(kernel, p, depth * n),
            out_shape=jax.ShapeDtypeStruct((count, depth), BF16),
            in_specs=[hbm] + [vmem] * 4 + [hbm] * 6,
            out_specs=hbm,
            scratch_shapes=scratch,
            compiler_params=pltpu.CompilerParams(
                collective_id=0, has_side_effects=True, vmem_limit_bytes=62 * 1024 * 1024
            ),
            name="both",
        )(tokens, row(pre1), row(post1), row(pre2), row(post2), gate1, up1, down1, gate2, up2, down2)

    in_specs = (
        P(None, "ra"), P("ra"), P("ra", "cb"), P("ra", "cb"), P("cb", "ra"), P("ra"),
        P("ra"), P("ra", "cb"), P("ra", "cb"), P("cb", "ra"), P("ra"),
    )
    return jax.shard_map(body, mesh=mesh, in_specs=in_specs, out_specs=P(None, "ra"), check_vma=False)
```

```python
import functools

import jax
import jax.numpy as jnp
from jax import lax
from jax.experimental import pallas as pl
from jax.experimental.pallas import tpu as pltpu
from jax.sharding import PartitionSpec as P

EPS = 1e-06
MESH = pl.DeviceIdType.MESH
F32 = jnp.float32
BF16 = jnp.bfloat16
LY, LZ, MY, MZ = 3, 3, 3, 3
POST = (1, 3, 5)


def log2(n):
    return n.bit_length() - 1


def spread(col):
    return jnp.broadcast_to(col, (col.shape[0], 128)).T[0:1]


def column(row):
    return jnp.broadcast_to(row, (128, row.shape[1])).T


class Plan:
    def __init__(self, n, nc, tokens, depth, hidden):
        self.n, self.nc, self.tokens, self.depth = n, nc, tokens, depth
        self.ny = 1 << (log2(n) // 2)
        self.nz = n // self.ny
        self.kx = log2(nc) - 1
        self.tb = 64 * self.ny
        self.half, self.g = self.tb // 2, 16
        self.lanes = max(self.half, 128)
        self.cw = 256 if hidden % 256 == 0 else 128
        self.chunks, self.blocks = hidden // self.cw, tokens // self.tb
        self.items = self.chunks * self.blocks
        self.act = (self.nz - 1) * LZ + LY
        self.down = self.act + MY + (self.nz - 1) * MZ
        steps = [0, POST[0]] + [POST[1]] * self.kx + [POST[2]]
        self.post = [self.down + sum(steps[: i + 1]) for i in range(len(steps))]
        self.gap = max(0, self.chunks + self.post[-1] - self.items)
        self.ticks = 2 * self.items + self.gap + self.post[-1]
        self.ring = self.items + self.gap + max(LY, MY)


def kernel(p, width, *refs):
    (tok_hbm, pre1, post1, pre2, post2, gate1, up1, down1, gate2, up2, down2, y_hbm), refs = refs[:12], refs[12:]
    (both_v, down_v, h_v, mid, acc, branch, scale, hid), refs = refs[:8], refs[8:]
    (yr_snd, yr_rcv, zr_snd, zr_rcv, ya_snd, ya_rcv, za), refs = refs[:7], refs[7:]
    (d_rcv, x_snd, x_rcv, tot, br_snd, br_rcv, ms_snd, ms_rcv), refs = refs[:8], refs[8:]
    (w_sem, yr_s, yr_r, zr_s, zr_r, ya_s, ya_r, za_s, za_r), refs = refs[:9], refs[9:]
    d_s, d_r, x_s, x_r, t_s, t_r, br_s, br_r, ms_s, ms_r, fac, tok, y_out, io_s = refs

    n, nc, ny, nz, tb, half, g, cw = p.n, p.nc, p.ny, p.nz, p.tb, p.half, p.g, p.cw
    chunks, blocks, items = p.chunks, p.blocks, p.items
    me, col = lax.axis_index("ra"), lax.axis_index("cb")
    z, y = lax.div(me, ny), lax.rem(me, ny)
    core = lax.rem(col, 2)
    brow = ny * g

    def remote(src, dst, s, r, **where):
        return pltpu.make_async_remote_copy(
            src_ref=src, dst_ref=dst, send_sem=s, recv_sem=r, device_id=where, device_id_type=MESH
        )

    def rows(base, size):
        return pl.ds(pl.multiple_of(base, 16), size)

    def weights(layer, c):
        cols = pl.ds(pl.multiple_of(c * cw, 128), cw)
        gate, up, down = ((gate1, up1, down1), (gate2, up2, down2))[layer]
        k = layer * chunks + c
        return [
            pltpu.make_async_copy(gate.at[:, cols], both_v.at[k, :, pl.ds(0, cw)], w_sem.at[0, k]),
            pltpu.make_async_copy(up.at[:, cols], both_v.at[k, :, pl.ds(cw, cw)], w_sem.at[1, k]),
            pltpu.make_async_copy(down.at[cols, :], down_v.at[k], w_sem.at[2, k]),
        ]

    def fetch(layer, start):
        @pl.loop(start, chunks)
        def _(c):
            for copy in weights(layer, c):
                copy.start()

    tok_copy = pltpu.make_async_copy(tok_hbm, tok, io_s.at[0])
    tok_copy.start()
    for copy in weights(0, 0):
        copy.start()
    barrier = pltpu.get_barrier_semaphore()
    for off in range(1, n):
        pl.semaphore_signal(barrier, inc=1, device_id={"ra": lax.rem(me + off, n)}, device_id_type=MESH)
    for off in range(1, nc):
        pl.semaphore_signal(barrier, inc=1, device_id={"cb": lax.rem(col + off, nc)}, device_id_type=MESH)

    fetch(0, 1)

    def other_y(j):
        return z * ny + lax.rem(y + j, ny)

    def next_z(e):
        return lax.rem(z + (1 if e else nz - 1), nz) * ny + y

    def back_z(e):
        return lax.rem(z + (nz - 1 if e else 1), nz) * ny + y

    def place(e):
        return z if e else nz - 1 - z

    def yr_copy(slot, j, part):
        return remote(
            yr_snd.at[slot, j - 1, pl.ds(*part), :], yr_rcv.at[slot, ny - 1 - j, pl.ds(*part), :],
            yr_s.at[j - 1, slot], yr_r.at[ny - 1 - j, slot], ra=other_y(j),
        )

    def ya_copy(slot, j, part):
        return remote(
            ya_snd.at[slot, pl.ds(*part), :], ya_rcv.at[slot, ny - 1 - j, pl.ds(*part), :],
            ya_s.at[j - 1, slot], ya_r.at[ny - 1 - j, slot], ra=other_y(j),
        )

    def zr_copy(slot, e, part):
        there = (slot, e, pl.ds(*part), slice(None))
        return remote(zr_snd.at[there], zr_rcv.at[there], zr_s.at[e, slot], zr_r.at[e, slot], ra=next_z(e))

    def za_copy(slot, e, part):
        there = za.at[slot, e, pl.ds(*part), :]
        return remote(there, there, za_s.at[e, slot], za_r.at[e, slot], ra=back_z(e))

    def by_type(both, here, act):
        for ok, part in ((both[0] & both[1], (0, brow + g)), (both[0] & ~both[1], (0, brow)), (both[1] & ~both[0], (brow, g))):
            @pl.when(ok & here)
            def _():
                act(part)

    def by_part(one, two, act):
        for ok, part in ((one & two, (0, 3 * g)), (one & ~two, (0, 2 * g)), (two & ~one, (2 * g, g))):
            @pl.when(ok)
            def _():
                for j in range(1, ny):
                    act(j, part)

    def ms_copy(layer, b, off):
        return remote(
            ms_snd.at[layer, b], ms_rcv.at[layer, b, n - 1 - off],
            ms_s.at[layer, b, off - 1], ms_r.at[layer, b, n - 1 - off], ra=lax.rem(me + off, n),
        )

    def br_copy(layer, b, off, across):
        start = n - 1 if across else -1
        to = start + (n - off) % n
        where = {"cb": col + 1 - 2 * core} if across else {}
        return remote(
            br_snd.at[layer, b], br_rcv.at[layer, b, to],
            br_s.at[layer, b, start + off], br_r.at[layer, b, to], ra=lax.rem(me + off, n), **where,
        )

    br_all = [(off, False) for off in range(1, n)] + [(off, True) for off in range(n)]

    def store_h(b, value):
        value = value.astype(BF16)
        for e in range(2):
            h_v[rows(b * tb + e * half, brow), :] = value[e * half : e * half + brow]
            for yy in range(ny):
                slot = lax.rem(yy - y + ny, ny)
                at = e * half + brow + yy * g
                h_v[rows(b * tb + e * half + brow + slot * g, g), :] = value[at : at + g]

    def squares(value):
        return spread(jnp.sum(value * value, axis=1, keepdims=True))

    def block_rows(b):
        return pl.ds(pl.multiple_of(b * tb, tb), tb)

    def start_blocks(b):
        value = tok[block_rows(b), :].astype(F32)
        mid[block_rows(b), :] = value
        ms_snd[0, b] = squares(value)

    tok_copy.wait()
    for b in range(blocks):
        start_blocks(b)
    store_h(0, mid[0:tb, :] * pre1[...])

    pl.semaphore_wait(barrier, n - 1 + nc - 1)

    def factor_of(layer, b):
        for off in range(1, n):
            ms_copy(layer, b, off).wait()
        total = ms_snd[layer, b]
        for off in range(1, n):
            total = total + ms_rcv[layer, b, off - 1]
        return column(lax.rsqrt(total / width + EPS))

    def prepare():
        for b in range(blocks):
            factor = factor_of(0, b)
            if b == 0:
                scale[block_rows(b), :] = factor
            else:
                scale[block_rows(b), :] = jnp.ones_like(factor)
                store_h(b, mid[block_rows(b), :] * factor[:, 0:1] * pre1[...])

    is_end = (z == 0) | (z == nz - 1)
    end = jnp.where(z == 0, 0, 1)
    last = nz - 1

    def item(u):
        later = u >= items + p.gap
        valid = ((u >= 0) & (u < items)) | (later & (u < 2 * items + p.gap))
        s = u - jnp.where(later, items + p.gap, 0)
        layer = jnp.where(later, 1, 0)
        b = lax.div(s, chunks)
        return valid, s, layer, b, s - b * chunks

    def y_copy(b):
        return pltpu.make_async_copy(y_out.at[block_rows(b), :], y_hbm.at[block_rows(b), :], io_s.at[1 + b])

    def slot_of(v):
        return lax.rem(jnp.maximum(v, 0), p.ring)

    def valid(u):
        return item(u)[0]

    def tick(t, carry):
        x = t - p.act
        y_slot, y_old = slot_of(t), slot_of(t - LY)
        g_slot, g_old = slot_of(x), slot_of(x - MY)

        @pl.when(t == chunks // 2)
        def _():
            prepare()
            fetch(1, 0)

        ok, s, layer, b, c = item(t)

        @pl.when(ok)
        def _():
            for one in range(2):
                @pl.when((b == 0) & (layer == one))
                def _():
                    gate_copy, up_copy, _ = weights(one, c)
                    gate_copy.wait()
                    up_copy.wait()
            value = jnp.dot(h_v[block_rows(b), :], both_v[layer * chunks + c], preferred_element_type=F32)
            for e in range(2):
                at = e * half + brow
                acc[s, e * half : at + g, :] = value[e * half : at + g]
                for j in range(1, ny):
                    yr_snd[y_slot, j - 1, e * g : (e + 1) * g, :] = value[at + j * g : at + (j + 1) * g].astype(BF16)

        by_part(
            valid(t - LY), is_end & valid(t - LY - last * LZ), lambda j, part: yr_copy(y_old, j, part).wait()
        )
        ok1, s1, _, _, _ = item(t - LY)

        @pl.when(ok1)
        def _():
            for e in range(2):
                mine = pl.ds(e * half + brow, g)
                total = acc[s1, mine, :]
                for j in range(1, ny):
                    total = total + yr_rcv[y_old, j - 1, e * g : (e + 1) * g, :].astype(F32)
                acc[s1, mine, :] = total

        for e in range(2):
            at = place(e)
            v = t - at * LZ
            now, old = slot_of(v), slot_of(v - LZ)
            ok_b, s_b, _, _, _ = item(v)
            ok_a, s_a, _, _, _ = item(v - LY)

            by_type((ok_b, ok_a), at > 0, lambda part: zr_copy(now, e, part).wait_recv())

            for ok_i, s_i, base, size in ((ok_b, s_b, 0, brow), (ok_a, s_a, brow, g)):
                mine, part = pl.ds(e * half + base, size), pl.ds(base, size)

                @pl.when(ok_i & (at == 0))
                def _():
                    zr_snd[now, e, part, :] = acc[s_i, mine, :].astype(BF16)

                @pl.when(ok_i & (at > 0) & (at < last))
                def _():
                    zr_snd[now, e, part, :] = (
                        acc[s_i, mine, :] + zr_rcv[now, e, part, :].astype(F32)
                    ).astype(BF16)

                @pl.when(ok_i & (at == last))
                def _():
                    acc[s_i, mine, :] += zr_rcv[now, e, part, :].astype(F32)

            by_type((ok_b, ok_a), at < last, lambda part: zr_copy(now, e, part).start())
            by_type(
                (valid(v - LZ), valid(v - LZ - LY)), at < last, lambda part: zr_copy(old, e, part).wait_send()
            )

        ok2, s2, _, _, _ = item(t - last * LZ)

        @pl.when(ok2 & is_end)
        def _():
            for j in range(1, ny):
                there = rows(end * half + lax.rem(y + j, ny) * g, g)
                yr_snd[y_slot, j - 1, 2 * g :, :] = acc[s2, there, :].astype(BF16)

        by_part(ok, ok2 & is_end, lambda j, part: yr_copy(y_slot, j, part).start())

        ok3, s3, layer3, b3, c3 = item(x)

        @pl.when(ok3 & (c3 == 0) & (layer3 == 1))
        def _():
            scale[block_rows(b3), :] = factor_of(1, b3)

        @pl.when(ok3 & is_end)
        def _():
            def activate(value, row):
                factor = scale[rows(b3 * tb + row, g), 0:1]
                gv, uv = value[:, :cw] * factor, value[:, cw:] * factor
                return (gv / (1.0 + jnp.exp(-gv)) * uv).astype(BF16)

            own = end * half + y * g
            total = acc[s3, rows(own, g), :]
            for j in range(1, ny):
                total = total + yr_rcv[y_old, j - 1, 2 * g :, :].astype(F32)
            value = activate(total, own)
            hid[s3, rows(own, g), :] = value
            ya_snd[g_slot, 2 * g :, :] = value
            own = rows(end * half + brow, g)
            hid[s3, own, :] = activate(acc[s3, own, :], end * half + brow + y * g)

        by_part(
            valid(x - MY - last * MZ), is_end & valid(x - MY), lambda j, part: ya_copy(g_old, j, part).wait()
        )
        ok4, s4, layer4, b4, c4 = item(t - p.down)
        ok5, s5, _, _, _ = item(x - MY)

        @pl.when(ok4)
        def _():
            for e in range(2):
                for j in range(1, ny):
                    to = e * half + brow + j * g
                    hid[s4, to : to + g, :] = ya_rcv[g_old, j - 1, e * g : (e + 1) * g, :]

        @pl.when(ok5 & is_end)
        def _():
            for j in range(1, ny):
                hid[s5, rows(end * half + lax.rem(y + j, ny) * g, g), :] = ya_rcv[g_old, j - 1, 2 * g :, :]

        for e in range(2):
            far = last - place(e)
            w = x - far * MZ
            now, old = slot_of(w), slot_of(w - MZ)
            ok_a, s_a, _, _, _ = item(w)
            ok_b, s_b, _, _, _ = item(w - MY)

            by_type((ok_b, ok_a), far > 0, lambda part: za_copy(now, e, part).wait_recv())

            for ok_i, s_i, base, size in ((ok_b, s_b, 0, brow), (ok_a, s_a, brow, g)):
                mine, part = pl.ds(e * half + base, size), pl.ds(base, size)

                @pl.when(ok_i & (far == 0))
                def _():
                    za[now, e, part, :] = hid[s_i, mine, :]

            by_type((ok_b, ok_a), far < last, lambda part: za_copy(now, e, part).start())

            for ok_i, s_i, base, size in ((ok_b, s_b, 0, brow), (ok_a, s_a, brow, g)):
                mine, part = pl.ds(e * half + base, size), pl.ds(base, size)

                @pl.when(ok_i & (far > 0))
                def _():
                    hid[s_i, mine, :] = za[now, e, part, :]

            by_type(
                (valid(w - MZ - MY), valid(w - MZ)), far < last, lambda part: za_copy(old, e, part).wait_send()
            )

        ok6, s6, _, _, _ = item(x - last * MZ)

        @pl.when(ok6)
        def _():
            for e in range(2):
                at = e * half + brow
                ya_snd[g_slot, e * g : (e + 1) * g, :] = hid[s6, at : at + g, :]

        by_part(ok6, ok3 & is_end, lambda j, part: ya_copy(g_slot, j, part).start())

        @pl.when(ok4)
        def _():
            for one in range(2):
                @pl.when((b4 == 0) & (layer4 == one))
                def _():
                    weights(one, c4)[2].wait()
            value = jnp.dot(hid[s4], down_v[layer4 * chunks + c4], preferred_element_type=F32)

            @pl.when(c4 == 0)
            def _():
                branch[block_rows(b4), :] = value

            @pl.when(c4 > 0)
            def _():
                branch[block_rows(b4), :] += value

        @pl.when(t == 0)
        def _():
            for b in range(blocks):
                for off in range(1, n):
                    ms_copy(0, b, off).start()

        def after(k):
            ok, _, layer, b, c = item(t - p.post[k])
            return ok & (c == chunks - 1), layer, b

        peer = col + 1 - 2 * core

        def d_copy(layer, b):
            away = branch.at[rows(b * tb + (1 - core) * half, half), :]
            return remote(away, d_rcv.at[layer, b], d_s.at[layer, b], d_r.at[layer, b], cb=peer)

        def x_copy(layer, b, k):
            bit = lax.rem(lax.div(col, 2 << k), 2)
            to = col + (1 - 2 * bit) * (2 << k)
            return remote(x_snd.at[layer, b, k], x_rcv.at[layer, b, k], x_s.at[layer, b, k], x_r.at[layer, b, k], cb=to)

        def t_copy(layer, b):
            part = tot.at[layer, b, rows(core * half, half), :]
            return remote(part, part, t_s.at[layer, b], t_r.at[layer, b], cb=peer)

        def whole(layer, b, total):
            base = core * half
            tot[layer, b, rows(base, brow), :] = total[:brow]
            for j in range(ny):
                to = base + brow + lax.rem(y + j, ny) * g
                tot[layer, b, rows(to, g), :] = total[brow + j * g : brow + (j + 1) * g]
            t_copy(layer, b).start()
            value = tot[layer, b, rows(base, half), :]
            sums = jnp.sum(value * value, axis=1, keepdims=True)
            if p.lanes > half:
                sums = jnp.concatenate([sums, jnp.zeros((p.lanes - half, 1), F32)], axis=0)
            br_snd[layer, b] = spread(sums)
            for off, across in br_all:
                br_copy(layer, b, off, across).start()

        go, layer, b = after(0)

        @pl.when(go)
        def _():
            d_copy(layer, b).start()

        for k in range(p.kx + 1):
            go_k, layer_k, b_k = after(k + 1)

            @pl.when(go_k)
            def _():
                if k == 0:
                    d_copy(layer_k, b_k).wait()
                    total = branch[rows(b_k * tb + core * half, half), :] + d_rcv[layer_k, b_k]
                else:
                    x_copy(layer_k, b_k, k - 1).wait()
                    total = x_snd[layer_k, b_k, k - 1].astype(F32) + x_rcv[layer_k, b_k, k - 1].astype(F32)
                if k < p.kx:
                    x_snd[layer_k, b_k, k] = total.astype(BF16)
                    x_copy(layer_k, b_k, k).start()
                else:
                    whole(layer_k, b_k, total)

        go6, layer6, b6 = after(p.kx + 2)

        for one in range(2):
            @pl.when(go6 & (layer6 == one))
            def _():
                t_copy(one, b6).wait()
                for off, across in br_all:
                    br_copy(one, b6, off, across).wait()
                own, other = br_snd[one, b6], br_rcv[one, b6, n - 1]
                for off in range(1, n):
                    own = own + br_rcv[one, b6, off - 1]
                    other = other + br_rcv[one, b6, n - 1 + off]
                for base, total in ((core * half, own), ((1 - core) * half, other)):
                    fac[rows(base, half), :] = column(0.5 * lax.rsqrt(total / width + EPS))[:half]
                factor = fac[:, 0:1]
                gain = (post1, post2)[one][...]
                middle = mid[block_rows(b6), :] + factor * tot[one, b6] * gain
                if one == 0:
                    mid[block_rows(b6), :] = middle
                    store_h(b6, middle * pre2[...])
                    ms_snd[1, b6] = squares(middle)
                    for off in range(1, n):
                        ms_copy(1, b6, off).start()
                else:
                    y_out[block_rows(b6), :] = middle.astype(BF16)
                    y_copy(b6).start()

        return carry

    lax.fori_loop(0, p.ticks, tick, 0)
    for b in range(blocks):
        y_copy(b).wait()


def solution(mesh):
    n, nc = mesh.shape["ra"], mesh.shape["cb"]

    def body(tokens, pre1, gate1, up1, down1, post1, pre2, gate2, up2, down2, post2):
        count, depth = tokens.shape
        p = Plan(n, nc, count, depth, gate1.shape[1])
        vmem = pl.BlockSpec(memory_space=pltpu.VMEM)
        hbm = pl.BlockSpec(memory_space=pl.ANY)
        dma = pltpu.SemaphoreType.DMA
        items, blocks, wide, ny = p.items, p.blocks, 2 * p.cw, p.ny
        scratch = [
            pltpu.VMEM((2 * p.chunks, depth, wide), BF16),
            pltpu.VMEM((2 * p.chunks, p.cw, depth), BF16),
            pltpu.VMEM((count, depth), BF16),
            pltpu.VMEM((count, depth), F32),
            pltpu.VMEM((items, p.tb, wide), F32),
            pltpu.VMEM((count, depth), F32),
            pltpu.VMEM((count, 128), F32),
            pltpu.VMEM((items, p.tb, p.cw), BF16),
        ]
        ring, many = p.ring, (ny + 1) * p.g
        scratch += [pltpu.VMEM((ring, ny - 1, 3 * p.g, wide), BF16)] * 2
        scratch += [pltpu.VMEM((ring, 2, many, wide), BF16)] * 2
        scratch += [pltpu.VMEM((ring, 3 * p.g, p.cw), BF16), pltpu.VMEM((ring, ny - 1, 3 * p.g, p.cw), BF16)]
        scratch += [pltpu.VMEM((ring, 2, many, p.cw), BF16)]
        scratch += [pltpu.VMEM((2, blocks, p.half, depth), F32)]
        scratch += [pltpu.VMEM((2, blocks, max(1, p.kx), p.half, depth), BF16)] * 2
        scratch += [pltpu.VMEM((2, blocks, p.tb, depth), F32)]
        scratch += [pltpu.VMEM((2, blocks, 1, p.lanes), F32), pltpu.VMEM((2, blocks, 2 * n - 1, 1, p.lanes), F32)]
        scratch += [pltpu.VMEM((2, blocks, 1, p.tb), F32), pltpu.VMEM((2, blocks, n - 1, 1, p.tb), F32)]
        scratch += [dma((3, 2 * p.chunks))]
        scratch += ([dma((ny - 1, ring))] * 2 + [dma((2, ring))] * 2) * 2
        scratch += [dma((2, blocks))] * 2 + [dma((2, blocks, max(1, p.kx)))] * 2 + [dma((2, blocks))] * 2
        scratch += [dma((2, blocks, 2 * n - 1))] * 2 + [dma((2, blocks, n - 1))] * 2
        scratch += [pltpu.VMEM((p.tb, 128), F32)] + [pltpu.VMEM((count, depth), BF16)] * 2 + [dma((1 + blocks,))]
        row = lambda gain: gain.reshape(1, depth)
        return pl.pallas_call(
            functools.partial(kernel, p, depth * n),
            out_shape=jax.ShapeDtypeStruct((count, depth), BF16),
            in_specs=[hbm] + [vmem] * 4 + [hbm] * 6,
            out_specs=hbm,
            scratch_shapes=scratch,
            compiler_params=pltpu.CompilerParams(
                collective_id=0, has_side_effects=True, vmem_limit_bytes=62 * 1024 * 1024
            ),
            name="both",
        )(tokens, row(pre1), row(post1), row(pre2), row(post2), gate1, up1, down1, gate2, up2, down2)

    in_specs = (
        P(None, "ra"), P("ra"), P("ra", "cb"), P("ra", "cb"), P("cb", "ra"), P("ra"),
        P("ra"), P("ra", "cb"), P("ra", "cb"), P("cb", "ra"), P("ra"),
    )
    return jax.shard_map(body, mesh=mesh, in_specs=in_specs, out_specs=P(None, "ra"), check_vma=False)
```
